32 devices in a mesh: grp: 2 (over y), ep: 4 (over z), tp: 4 (over x, core).
Axes of the slice: x: 2, y: 2, z: 4, core: 2. Of those that a mesh axis runs over, the one named last changes fastest.
Arguments:
- mix_query: bfloat16 [4096, 16, 128], P(('grp', 'ep'), 'tp'), parts along dimension 0, may hold values from -6 to 6
- mix_keys: bfloat16 [4096, 16, 128], P(('grp', 'ep'), 'tp'), parts along dimension 0, may hold values from -6 to 6
- mix_values: bfloat16 [4096, 16, 128], P(('grp', 'ep'), 'tp'), parts along dimension 0, may hold values from -6 to 6
- beta_in: float32 [16, 4096], P('tp', ('grp', 'ep')), parts along dimension 1, may hold values from -9.5 to 6
- decay_in: float32 [16, 4096], P('tp', ('grp', 'ep')), parts along dimension 1, may hold values from -14 to 0
- norm_gain: float32 [128], replicated, may hold values from 0.1 to 1.9
- ffn_input: bfloat16 [1024, 4096], P(('grp', 'ep'), 'tp'), parts along dimension 0, may hold values from -200 to 200
- ffn_gain: float32 [4096], P('tp'), may hold values from 0.1 to 1.9
- expert_ids: int32 [1024, 2], P(('grp', 'ep')), parts along dimension 0, may hold values from 0 to 15, as said below
- expert_share: float32 [1024, 2], P(('grp', 'ep')), parts along dimension 0, may hold values from 0.2 to 1
- w_gate: bfloat16 [16, 4096, 1024], P('ep', None, 'tp'), may hold values from -0.09375 to 0.09375
- w_up: bfloat16 [16, 4096, 1024], P('ep', None, 'tp'), may hold values from -0.09375 to 0.09375
- w_down: bfloat16 [16, 1024, 4096], P('ep', None, 'tp'), may hold values from -0.1875 to 0.1875
Outputs:
- mix_out: bfloat16 [4096, 16, 128], P(('grp', 'ep'), 'tp'), parts along dimension 0
- ffn_out: bfloat16 [1024, 4096], P(('grp', 'ep'), 'tp'), parts along dimension 0
The draws below stay inside these ranges and needn't reach their ends.
There are 2 independent parts, one for each index of `grp`. The reference program is written for one: setup_inputs(seed, part) draws one part's arguments, and reference() takes and returns one part's arrays. A program takes and returns all parts, laid end to end along the dimension named above; an argument that names none is the same for every part. Nothing has to cross between parts.
Inputs may be any that keep to these rules, and one draw needn't show every extreme that they name: `expert_ids`: each row names two different experts of one group, the group being id // 4; the rows of one device (aligned blocks of 128 rows) name every expert exactly 2 * 128 // 16 times.
All inputs are finite; a program needn't handle non-finite values.
Results may differ from the reference program's by a relative error of at most 0.007.
Values may be sent and summed in bfloat16 or wider, within the bound.
No kernel may reach another device: no remote copies, remote signals or barrier semaphores. Data moves between devices by JAX's collectives and lax.ppermute only.
A program may use at most 128 MiB of HBM per device.

```python
import math
import jax
import jax.numpy as jnp
from jax import lax

D = 4096
HEADS = 16
HD = 128
BLOCK = 64
SEQ_DEV = 512
SEQUENCE_LENGTH = 2048
FF = 1024
GROUPS = 4
GROUP_SIZE = 4
EXPERTS = 16
RB_EP = 128
TB = 512


def draw_beta_in(key, part):
    token_sequence = jax.random.split(jax.random.fold_in(key, 11), 2)
    weak_heads = (jax.random.permutation(token_sequence[0], HEADS) < HEADS // 2)[:, None]
    centre = jnp.where(weak_heads, -5.3, 0.0)
    spread = jnp.where(weak_heads, 1.0, 1.5)
    noise = jax.random.truncated_normal(token_sequence[1], -4.0, 4.0, (HEADS, SEQUENCE_LENGTH), jnp.float32)
    return centre + spread * noise


def draw_decay_in(key, part):
    token_sequence = jax.random.split(key, 4)
    head_log_decay = jax.random.uniform(token_sequence[0], (HEADS, 1), jnp.float32, math.log(3e-05), math.log(0.03))
    span_count = 2 * (SEQUENCE_LENGTH // SEQ_DEV)
    span_index = jnp.arange(SEQUENCE_LENGTH) * span_count // SEQUENCE_LENGTH
    span_table = jnp.exp(jax.random.uniform(token_sequence[1], (HEADS, span_count), jnp.float32, math.log(0.5), math.log(2.0)))
    position_values = span_table[:, span_index]
    random_offset = jnp.exp(jax.random.uniform(token_sequence[2], (HEADS, SEQUENCE_LENGTH), jnp.float32, -0.5, 0.5))
    spike_position = jax.random.randint(token_sequence[3], (6,), 0, SEQUENCE_LENGTH)
    spike_tokens = jnp.any(jnp.arange(SEQUENCE_LENGTH)[None, :] == spike_position[:, None], axis=0).astype(jnp.float32)
    decay_rate_rows = jnp.exp(head_log_decay) * position_values * random_offset + 0.4 * spike_tokens[None, :]
    return jnp.log(jnp.expm1(decay_rate_rows))


def draw_ffn_input(key, part):
    token_sequence = jax.random.split(key, 3)
    columns = jnp.arange(D, dtype=jnp.float32) / D
    column_scale = jnp.exp(math.log(3.0) * columns + jax.random.uniform(token_sequence[0], (D,), jnp.float32, -0.4, 0.4))
    base_values = jax.random.truncated_normal(token_sequence[1], -4.0, 4.0, (TB, D), jnp.float32)
    row_scale = jnp.exp(jax.random.uniform(token_sequence[2], (TB, 1), jnp.float32, 0.0, math.log(10.0)))
    return (base_values * row_scale * column_scale[None, :]).astype(jnp.bfloat16)


def draw_expert_ids(key, part):
    source_count = TB // RB_EP
    block_keys = jax.random.split(key, source_count)
    rank_values = jax.vmap(lambda one_key: jax.random.permutation(one_key, RB_EP))(block_keys).reshape(-1)
    group_of = rank_values % GROUPS
    within = rank_values // GROUPS
    first_pick = within % GROUP_SIZE
    second = (first_pick + 1 + within // GROUP_SIZE % (GROUP_SIZE - 1)) % GROUP_SIZE
    return jnp.stack([group_of * GROUP_SIZE + first_pick, group_of * GROUP_SIZE + second], axis=1).astype(jnp.int32)


def block_levels(own_key, shape, pieces, smallest, largest):
    def one(dim, blocks):
        draws = jax.random.uniform(jax.random.fold_in(jax.random.fold_in(own_key, 6), dim), (blocks,), jnp.float32, smallest / len(pieces), largest / len(pieces))
        return jnp.repeat(jnp.exp(draws), shape[dim] // blocks).reshape((-1,) + (1,) * (len(shape) - dim - 1))

    loudness = one(*pieces[0])
    for cut in pieces[1:]:
        loudness = loudness * one(*cut)
    return loudness


def centred(stream_key, shape, scale, bound, cuts=(), held_as=jnp.bfloat16):
    factor_of = block_levels(stream_key, shape, cuts, -0.22, 0.18) if cuts else 1.0
    drawn = jax.random.normal(stream_key, shape, jnp.float32) * scale * factor_of
    return jnp.minimum(jnp.maximum(drawn, -bound), bound).astype(held_as)


def setup_inputs(seed: int = 0, part: int = 0) -> dict:
    streams_of = jax.random.split(jax.random.key(seed), 14)
    part_keys = jax.random.split(jax.random.fold_in(streams_of[13], part), 14)
    return {
        "mix_query": centred(part_keys[0], (SEQUENCE_LENGTH, HEADS, HD), 1.0, 6.0, ((0, 4), (1, 4))),
        "mix_keys": centred(part_keys[1], (SEQUENCE_LENGTH, HEADS, HD), 1.0, 6.0, ((0, 4), (1, 4))),
        "mix_values": centred(part_keys[2], (SEQUENCE_LENGTH, HEADS, HD), 1.0, 6.0, ((0, 4), (1, 4))),
        "beta_in": draw_beta_in(jax.random.fold_in(jax.random.fold_in(streams_of[13], part), 71), part),
        "decay_in": draw_decay_in(jax.random.fold_in(jax.random.fold_in(streams_of[13], part), 71), part),
        "norm_gain": jnp.clip(1.0 + 0.18 * jax.random.normal(streams_of[5], (HD,), jnp.float32), 0.1, 1.9),
        "ffn_input": draw_ffn_input(jax.random.fold_in(jax.random.fold_in(streams_of[13], part), 71), part),
        "ffn_gain": jnp.clip(1.0 + 0.18 * jax.random.normal(streams_of[7], (D,), jnp.float32), 0.1, 1.9),
        "expert_ids": draw_expert_ids(jax.random.fold_in(jax.random.fold_in(streams_of[13], part), 71), part),
        "expert_share": jnp.clip(0.2 + 0.8 * jax.random.uniform(part_keys[9], (TB, 2), jnp.float32) ** block_levels(part_keys[9], (TB, 2), ((0, 4),), -0.2, 0.2), 0.2, 1.0),
        "w_gate": centred(streams_of[10], (EXPERTS, D, FF), D ** -0.5, 0.09375, ((0, 4), (2, 4))),
        "w_up": centred(streams_of[11], (EXPERTS, D, FF), D ** -0.5, 0.09375, ((0, 4), (2, 4))),
        "w_down": centred(streams_of[12], (EXPERTS, FF, D), FF ** -0.5, 0.1875, ((0, 4), (2, 4))),
    }


PRECISE = lax.Precision.HIGHEST
EPSILON = 1e-06

def unit_inverse(strict_lower):
    extent = strict_lower.shape[-1]
    identity = jnp.eye(extent, dtype=jnp.float32)
    powered = -strict_lower
    product = identity + powered
    for section_index in range(1, (extent - 1).bit_length()):
        powered = jnp.matmul(powered, powered, precision=PRECISE)
        product = jnp.matmul(product, identity + powered, precision=PRECISE)
    return product

def block_terms(queries, keyset, valueset, betas, rates):
    extent = queries.shape[-2]
    cumulative = -jnp.cumsum(rates, axis=-1)
    positions = jnp.arange(extent)
    causal = positions[:, None] >= positions[None, :]
    strict = positions[:, None] > positions[None, :]
    spread = cumulative[..., :, None] - cumulative[..., None, :]
    decay_mask = jnp.where(causal, jnp.exp(jnp.where(causal, spread, 0.0)), 0.0)
    keys_beta = keyset * betas[..., None]
    values_beta = valueset * betas[..., None]
    lower_part = jnp.where(strict, jnp.einsum('...id,...jd->...ij', keys_beta, keyset, precision=PRECISE) * decay_mask, 0.0)
    inverse = unit_inverse(lower_part)
    update = jnp.einsum('...ij,...jd->...id', inverse, values_beta, precision=PRECISE)
    correction = jnp.einsum('...ij,...jd->...id', inverse, keys_beta * jnp.exp(cumulative)[..., None], precision=PRECISE)
    scores = jnp.where(causal, jnp.einsum('...id,...jd->...ij', queries, keyset, precision=PRECISE) * decay_mask, 0.0)
    query_decay = queries * jnp.exp(cumulative)[..., None]
    key_decay = keyset * jnp.exp(cumulative[..., -1:] - cumulative)[..., None]
    block_decay = jnp.exp(cumulative[..., -1])
    return (query_decay, key_decay, update, correction, scores, block_decay)

def unit_rows(values_in, factor):
    floats = values_in.astype(jnp.float32)
    return floats * lax.rsqrt(lax.optimization_barrier(jnp.sum(floats * floats, -1, keepdims=True)) + EPSILON) * factor

def mixer_reference(mix_query, mix_keys, mix_values, beta_in, decay_in, norm_gain):
    length, head_count, width = mix_query.shape
    blocks = length // BLOCK

    def to_blocks(tensor):
        return tensor.reshape(blocks, BLOCK, head_count, width).transpose(0, 2, 1, 3)
    queries = to_blocks(unit_rows(mix_query, width ** (-0.5)))
    keyset = to_blocks(unit_rows(mix_keys, 1.0))
    valueset = to_blocks(mix_values.astype(jnp.float32))
    betas = jax.nn.sigmoid(beta_in).reshape(head_count, blocks, BLOCK).transpose(1, 0, 2)
    rates = jax.nn.softplus(decay_in).reshape(head_count, blocks, BLOCK).transpose(1, 0, 2)

    def advance(carried, inputs):
        query_decay, key_decay, update, correction, scores, block_decay = block_terms(*inputs)
        fresh = update - jnp.einsum('hcd,hde->hce', correction, carried, precision=PRECISE)
        output = jnp.einsum('hcd,hde->hce', query_decay, carried, precision=PRECISE) + jnp.einsum('hij,hje->hie', scores, fresh, precision=PRECISE)
        carried = carried * block_decay[:, None, None] + jnp.einsum('hcd,hce->hde', key_decay, fresh, precision=PRECISE)
        return (carried, output)
    initial = jnp.zeros((head_count, width, width), jnp.float32)
    ignored, outputs = lax.scan(advance, initial, (queries, keyset, valueset, betas, rates))
    raw_mix = outputs.transpose(0, 2, 1, 3).reshape(length, head_count, width)
    return (raw_mix * lax.rsqrt(lax.optimization_barrier(jnp.mean(raw_mix * raw_mix, -1, keepdims=True)) + EPSILON) * norm_gain).astype(jnp.bfloat16)

def experts_reference(ffn_input, ffn_gain, expert_ids, expert_share, w_gate, w_up, w_down):
    floats = ffn_input.astype(jnp.float32)
    normed = (floats * lax.rsqrt(lax.optimization_barrier(jnp.mean(floats * floats, -1, keepdims=True)) + EPSILON) * ffn_gain).astype(jnp.bfloat16)
    pick_count = expert_ids.shape[1]
    flat_ids = expert_ids.reshape(-1)
    sort_order = jnp.argsort(flat_ids, stable=True).astype(jnp.int32)
    source_rows = (sort_order // pick_count).reshape(w_gate.shape[0], -1)

    def one_expert(inputs):
        rows_here, gate_weight, up_weight, down_weight = inputs
        chosen = normed[rows_here]
        gate_sum = jnp.dot(chosen, gate_weight, preferred_element_type=jnp.float32)
        up_sum = jnp.dot(chosen, up_weight, preferred_element_type=jnp.float32)
        hidden = (jax.nn.silu(gate_sum) * up_sum).astype(jnp.bfloat16)
        return jnp.dot(hidden, down_weight, preferred_element_type=jnp.float32).astype(jnp.bfloat16)
    copies = lax.map(one_expert, (source_rows, w_gate, w_up, w_down)).reshape(-1, normed.shape[1])
    slots = jnp.argsort(sort_order).astype(jnp.int32)
    per_slot = copies[slots].reshape(expert_ids.shape[0], pick_count, -1)
    return lax.optimization_barrier(jnp.sum(per_slot.astype(jnp.float32) * expert_share[..., None], axis=1)).astype(jnp.bfloat16)

def reference(mix_query, mix_keys, mix_values, beta_in, decay_in, norm_gain, ffn_input, ffn_gain, expert_ids, expert_share, w_gate, w_up, w_down):
    mix_out = mixer_reference(mix_query, mix_keys, mix_values, beta_in, decay_in, norm_gain)
    ffn_out = experts_reference(ffn_input, ffn_gain, expert_ids, expert_share, w_gate, w_up, w_down)
    return (mix_out, ffn_out)
```

```python
import functools

import jax
import jax.numpy as jnp
from jax import lax
from jax.experimental import pallas as pl
from jax.experimental.pallas import tpu as pltpu
from jax.sharding import PartitionSpec as P


EPSILON = 1e-06
GROUP = 4
F32 = jnp.float32
BF16 = jnp.bfloat16
INFO = 128
GAIN_AT = 32
MIX_VMEM = 12 * 2**20
SMALL_VMEM = 8 * 2**20


def mm(a, b):
    return jnp.dot(a, b, preferred_element_type=F32)


def mm_nt(a, b):
    return lax.dot_general(a, b, (((1,), (1,)), ((), ())), preferred_element_type=F32)


def mm_tn(a, b):
    return lax.dot_general(a, b, (((0,), (0,)), ((), ())), preferred_element_type=F32)


def split2(x):
    high = x.astype(BF16)
    return high, (x - high.astype(F32)).astype(BF16)


def split3(x):
    high, rest = x.astype(BF16), None
    rest = x - high.astype(F32)
    middle = rest.astype(BF16)
    return high, middle, (rest - middle.astype(F32)).astype(BF16)


def iota(shape, dim):
    return lax.broadcasted_iota(jnp.int32, shape, dim)


def is_power(n):
    return n > 0 and n & (n - 1) == 0


def in_hbm(arrays):
    return tuple(pltpu.with_memory_space_constraint(t, pltpu.HBM) for t in arrays)


def in_vmem(arrays):
    return tuple(pltpu.with_memory_space_constraint(t, pltpu.VMEM) for t in arrays)


def fetch_all(sources, targets, sems):
    copies = [pltpu.make_async_copy(s, t, sems.at[n]) for n, (s, t) in enumerate(zip(sources, targets))]
    for copy in copies:
        copy.start()
    return copies


def mix_local_kernel(heads, first, count, chunk, fetches, q_ref, k_ref, v_ref, beta_hbm, decay_hbm, *refs):
    earlier = refs[: 1 if first else 0]
    refs = refs[len(earlier) :]
    sources, refs = refs[:fetches], refs[fetches:]
    qe_ref, o_ref, state_ref = refs[:3]
    targets = refs[3 : 3 + fetches]
    masks, beta_ref, decay_ref, sems = refs[3 + fetches :]
    copies = fetch_all((beta_hbm, decay_hbm) + sources, (beta_ref, decay_ref) + targets, sems)
    for copy in copies[:2]:
        copy.wait()
    length = q_ref.shape[0]
    width = q_ref.shape[1] // heads
    chunks = length // chunk
    beta = 1.0 / (1.0 + jnp.exp(-beta_ref[...]))
    decay = decay_ref[...]
    rate = jnp.maximum(decay, 0.0) + jnp.log1p(jnp.exp(-jnp.abs(decay)))
    lane = iota(rate.shape, 1) % chunk
    cumulative = -rate
    step = 1
    while step < chunk:
        cumulative = cumulative + jnp.where(lane >= step, pltpu.roll(cumulative, step, 1), 0.0)
        step *= 2
    rows = jnp.concatenate([beta, cumulative], 0)
    pad = -rows.shape[0] % 8
    if pad:
        rows = jnp.concatenate([rows, jnp.zeros((pad, length), F32)], 0)
    columns = rows.T

    row_id, col_id = iota((chunk, chunk), 0), iota((chunk, chunk), 1)
    causal = row_id >= col_id
    strict = row_id > col_id
    eye = row_id == col_id
    pair = (row_id // 2 == col_id // 2) & strict
    sizes = []
    size = 2
    while size < chunk:
        masks[len(sizes)] = jnp.where(
            (row_id // (2 * size) == col_id // (2 * size)) & (row_id // size != col_id // size), 1.0, 0.0
        ).astype(BF16)
        sizes.append(size)
        size *= 2

    every = [(h, c) for c in range(chunks) for h in range(first, first + count)]
    at = {}
    for h, c in every:
        span = slice(c * chunk, (c + 1) * chunk)
        lanes = slice(h * width, (h + 1) * width)
        q, k = q_ref[span, lanes], k_ref[span, lanes]
        beta_col = columns[span, h : h + 1]
        cum_col = columns[span, heads + h : heads + h + 1]
        cum_row = cumulative[h : h + 1, span]
        kk = mm_nt(k, k)
        qk = mm_nt(q, k)
        diagonal = jnp.where(eye, kk, 0.0)
        rk_col = lax.rsqrt(jnp.sum(diagonal, 1, keepdims=True) + EPSILON)
        rk_row = lax.rsqrt(jnp.sum(diagonal, 0, keepdims=True) + EPSILON)
        qf = q.astype(F32)
        rq_col = lax.rsqrt(jnp.sum(qf * qf, 1, keepdims=True) + EPSILON) * width**-0.5
        decays = jnp.exp(jnp.where(causal, cum_col - cum_row, 0.0)) * rk_row
        lower = jnp.where(strict, kk * decays * (beta_col * rk_col), 0.0)
        scores = jnp.where(causal, qk * decays * rq_col, 0.0).astype(BF16)
        low16 = lower.astype(BF16)
        rest16 = (lower - low16.astype(F32)).astype(BF16)
        inv16 = (jnp.where(eye, 1.0, 0.0) - jnp.where(pair, lower, 0.0)).astype(BF16)
        at[h, c] = dict(
            q=q, k=k, beta=beta_col, cum=cum_col, rk=rk_col, rq=rq_col, low=low16, rest=rest16, scores=scores, inv=inv16
        )
    for level, size in enumerate(sizes):
        odd = size >= 16

        def take(x):
            if not odd:
                return x
            return jnp.concatenate([x[i : i + size] for i in range(size, chunk, 2 * size)], 0)

        def put(x):
            if not odd:
                return x
            zero = jnp.zeros((size, chunk), x.dtype)
            parts = []
            for i in range(0, chunk // 2, size):
                parts += [zero, x[i : i + size]]
            return jnp.concatenate(parts, 0)

        mask = take(masks[level])
        for key in every:
            s = at[key]
            s["part"] = mm(take(s["low"]) * mask, s["inv"]).astype(BF16)
        for key in every:
            s = at[key]
            s["inv"] = s["inv"] - put(mm(take(s["inv"]), put(s["part"])).astype(BF16))
    for key in every:
        s = at[key]
        product = mm(s["low"], s["inv"]) + mm(s["rest"], s["inv"])
        start = s["inv"].astype(F32)
        residual = jnp.where(eye, 1.0, 0.0) - start - product
        s["inv2"] = split2(start + mm(s["inv"], residual.astype(BF16)))
    state = {}
    for c in range(chunks):
        span = slice(c * chunk, (c + 1) * chunk)
        for h in range(first, first + count):
            s = at[h, c]
            lanes = slice(h * width, (h + 1) * width)
            own = slice((h - first) * width, (h - first + 1) * width)
            q, k = s["q"], s["k"]
            v = v_ref[span, lanes].astype(F32)
            grown = jnp.exp(s["cum"])
            k_scale = -s["beta"] * grown * s["rk"]
            if c == 0:
                right = jnp.concatenate([k.astype(F32) * k_scale, v * s["beta"]], 1)
                q_part = jnp.concatenate([q.astype(F32), jnp.zeros_like(v)], 1)
            else:
                state_high, state_low = split2(state[h])
                right = (mm(k, state_high) + mm(k, state_low)) * k_scale
                right = right + jnp.concatenate([jnp.zeros_like(v), v * s["beta"]], 1)
                q_part = mm(q, state_high) + mm(q, state_low)
            inv_high, inv_low = s["inv2"]
            right_high, right_low = split2(right)
            fresh = mm(inv_high, right_high) + mm(inv_high, right_low) + mm(inv_low, right_high)
            fresh_high, fresh_low = split2(fresh)
            out = q_part * (grown * s["rq"]) + mm(s["scores"], fresh_high) + mm(s["scores"], fresh_low)
            qe_ref[span, own] = out[:, :width].astype(BF16)
            o_ref[span, own] = out[:, width:]
            last = s["cum"][chunk - 1 : chunk]
            sent_high, sent_low = split2(fresh * (s["rk"] * jnp.exp(last - s["cum"])))
            new = mm_tn(k, sent_high) + mm_tn(k, sent_low)
            if c == 0:
                ident = jnp.where(iota((width, 2 * width), 0) == iota((width, 2 * width), 1), 1.0, 0.0)
                state[h] = ident * jnp.exp(last) + new
            else:
                state[h] = state[h] * jnp.exp(last) + new
    if first:
        state_ref[:first] = earlier[0][...]
    for h in range(first, first + count):
        state_ref[h] = state[h].astype(BF16)
    for copy in copies[2:]:
        copy.wait()


def mix_local(heads, first, count, q, k, v, beta_in, decay_in, earlier=None, fetch=()):
    length, wide = q.shape
    width = wide // heads
    chunk = 1
    while chunk < 256 and length % (2 * chunk) == 0:
        chunk *= 2
    levels = max(chunk.bit_length() - 2, 1)
    args = (q, k, v) + in_hbm((beta_in, decay_in)) + ((earlier,) if first else ()) + in_hbm(fetch)
    vmem, hbm = (pl.BlockSpec(memory_space=s) for s in (pltpu.VMEM, pltpu.HBM))
    return pl.pallas_call(
        functools.partial(mix_local_kernel, heads, first, count, chunk, len(fetch)),
        out_shape=(
            jax.ShapeDtypeStruct((length, count * width), BF16),
            jax.ShapeDtypeStruct((length, count * width), F32),
            jax.ShapeDtypeStruct((first + count, width, 2 * width), BF16),
            *(pltpu.VMEM(t.shape, t.dtype) for t in fetch),
        ),
        in_specs=[vmem] * 3 + [hbm] * 2 + [vmem] * (1 if first else 0) + [hbm] * len(fetch),
        out_specs=(vmem,) * (3 + len(fetch)),
        scratch_shapes=[
            pltpu.VMEM((levels, chunk, chunk), BF16),
            pltpu.VMEM(beta_in.shape, F32),
            pltpu.VMEM(decay_in.shape, F32),
            pltpu.SemaphoreType.DMA((2 + len(fetch),)),
        ],
        compiler_params=pltpu.CompilerParams(vmem_limit_bytes=MIX_VMEM),
        name="mix_local",
    )(*args)


def join_kernel(later_ref, earlier_ref, *outs):
    heads, width, _ = later_ref.shape
    for h in range(heads):
        both = mm(later_ref[h, :, :width], earlier_ref[h])
        add = later_ref[h, :, width:].astype(F32) + both[:, width:]
        if len(outs) == 1 and outs[0].shape[2] == width:
            outs[0][h] = add.astype(BF16)
        else:
            outs[0][h] = jnp.concatenate([both[:, :width], add], 1).astype(BF16)


def join(later, earlier, with_map):
    heads, width, double = later.shape
    return pl.pallas_call(
        join_kernel,
        out_shape=jax.ShapeDtypeStruct((heads, width, double if with_map else width), BF16),
        compiler_params=pltpu.CompilerParams(vmem_limit_bytes=SMALL_VMEM),
        name="join",
    )(later, earlier)


def mix_finish_kernel(halves, latest_ref, *refs):
    add_ref = refs[0] if halves[0] else None
    refs = refs[1:] if halves[0] else refs
    gain_ref, out_ref = refs[-2:]
    width = latest_ref.shape[1]
    gain = gain_ref[...]
    h = 0
    for part, count in enumerate(halves[1]):
        qe_ref, o_ref = refs[2 * part : 2 * part + 2]
        for own in range(count):
            lanes = slice(own * width, (own + 1) * width)
            if add_ref is not None:
                entering = latest_ref[h, :, width:].astype(F32) + mm(latest_ref[h, :, :width], add_ref[h])
                entering = entering.astype(BF16)
            else:
                entering = latest_ref[h, :, width:]
            raw = o_ref[:, lanes] + mm(qe_ref[:, lanes], entering)
            scale = lax.rsqrt(jnp.sum(raw * raw, 1, keepdims=True) * (1.0 / width) + EPSILON)
            out_ref[:, h * width : (h + 1) * width] = (raw * scale * gain).astype(BF16)
            h += 1


def mix_finish(parts, latest, earlier, norm_gain):
    width = latest.shape[1]
    counts = tuple(p[0].shape[1] // width for p in parts)
    args = [latest] + ([] if earlier is None else [earlier]) + [t for p in parts for t in p] + [norm_gain[None, :]]
    return pl.pallas_call(
        functools.partial(mix_finish_kernel, (earlier is not None, counts)),
        out_shape=jax.ShapeDtypeStruct((parts[0][0].shape[0], sum(counts) * width), BF16),
        compiler_params=pltpu.CompilerParams(vmem_limit_bytes=SMALL_VMEM),
        name="mix_finish",
    )(*args)


def mixer_start(mix_query, mix_keys, mix_values, beta_in, decay_in, early, late):
    length, heads, width = mix_query.shape
    flat = [t.reshape(length, heads * width) for t in (mix_query, mix_keys, mix_values)]
    half = max(heads // 2, 1)
    if half == heads:
        early, late = early + late, ()
    got = mix_local(heads, 0, half, *flat, beta_in, decay_in, fetch=early)
    parts, own, fetched = [got[:2]], got[2], got[3:]
    if half < heads:
        got = mix_local(heads, half, heads - half, *flat, beta_in, decay_in, own, late)
        parts, own, fetched = parts + [got[:2]], got[2], fetched + got[3:]
    return parts, own, fetched


def mixer_end(parts, own, norm_gain):
    width = own.shape[1]
    count = lax.axis_size("ep")
    inclusive, latest, earlier = own, jnp.zeros_like(own), None
    shift = 1
    while shift < count:
        line = [(i, i + shift) for i in range(count - shift)]
        if earlier is not None:
            latest = join(latest, earlier, True)
        sent = inclusive
        if 2 * shift >= count and shift > 1 and inclusive.shape[2] > width:
            sent = inclusive[:, :, width:]
        arrived = lax.ppermute(sent, "ep", line)
        if shift == 1:
            latest = arrived
        else:
            earlier = arrived
        if 2 * shift < count:
            inclusive = join(inclusive, arrived, 4 * shift < count)
        shift *= 2
    out = mix_finish(parts, latest, earlier, norm_gain)
    return out.reshape(out.shape[0], own.shape[0], width)


def to_row(col, eye):
    return jnp.sum(jnp.where(eye, col, 0.0), 0, keepdims=True)


def to_col(row, eye):
    return jnp.sum(jnp.where(eye, row, 0.0), 1, keepdims=True)


def scatter_kernel(parts, owned, use_xor, me_ref, other_ref, ids_hbm, share_hbm, x_hbm, gain_hbm, perm_ref, *refs):
    outs = refs[:parts]
    ids_ref, share_ref, x_ref, gain_ref, sems = refs[parts:]
    copies = fetch_all((ids_hbm, share_hbm, x_hbm, gain_hbm), (ids_ref, share_ref, x_ref, gain_ref), sems)
    for copy in copies:
        copy.wait()
    rows, width = x_ref.shape
    per_part = rows // parts
    me = me_ref[0]
    x = x_ref[...].astype(F32)
    squares = jnp.sum(x * x, 1, keepdims=True)
    ids = ids_ref[...]
    share = share_ref[...]
    target = ids[0:1] // owned
    local = (ids - target * owned).astype(F32)
    block_row = (target ^ me if use_xor else (target - me + parts) % parts).astype(F32)
    row_id, col_id = iota((rows, rows), 0), iota((rows, rows), 1)
    eye = row_id == col_id
    before = jnp.where((to_col(block_row, eye) == block_row) & (row_id < col_id), 1.0, 0.0)
    slot_row = block_row * per_part + jnp.sum(before, 0, keepdims=True)
    perm = jnp.where(slot_row == row_id.astype(F32), 1.0, 0.0).astype(BF16)
    perm_ref[...] = perm
    known = [local[0:1], local[1:2], *split3(share[0:1]), *split3(share[1:2]), *split3(to_row(squares, eye))]
    known = jnp.concatenate([t.astype(F32) for t in known] + [jnp.zeros((INFO - len(known), rows), F32)], 0)
    info = mm_nt(perm, known.astype(BF16))
    moved = mm(perm, x_ref[...]).astype(BF16)
    cols = width // per_part
    own_row = iota((per_part, width), 1) // cols == iota((per_part, width), 0)
    lane, place = iota((width, INFO), 0) % cols, iota((width, INFO), 1)
    packed = jnp.zeros((per_part, INFO), F32)
    for n, piece in enumerate(split3(gain_ref[...])):
        fold = jnp.where(place == lane + (GAIN_AT + n * cols), 1.0, 0.0).astype(BF16)
        packed = packed + mm(jnp.where(own_row, piece.astype(F32), 0.0).astype(BF16), fold)
    for part in range(parts):
        span = slice(part * per_part, (part + 1) * per_part)
        outs[part][:, :width] = moved[span]
        outs[part][:, width:] = (info[span] + packed if part == 0 else info[span]).astype(BF16)


def scatter_rows(parts, owned, use_xor, me, other, expert_ids, expert_share, ffn_input, ffn_gain):
    rows, width = ffn_input.shape
    piece = jax.ShapeDtypeStruct((rows // parts, width + INFO), BF16)
    got = pl.pallas_call(
        functools.partial(scatter_kernel, parts, owned, use_xor),
        out_shape=(jax.ShapeDtypeStruct((rows, rows), BF16),) + (piece,) * parts,
        in_specs=[pl.BlockSpec(memory_space=pltpu.SMEM)] * 2 + [pl.BlockSpec(memory_space=pltpu.HBM)] * 4,
        scratch_shapes=[
            pltpu.VMEM(expert_ids.shape[::-1], jnp.int32),
            pltpu.VMEM(expert_share.shape[::-1], F32),
            pltpu.VMEM((rows, width), BF16),
            pltpu.VMEM((1, width), F32),
            pltpu.SemaphoreType.DMA((4,)),
        ],
        compiler_params=pltpu.CompilerParams(vmem_limit_bytes=SMALL_VMEM),
        name="scatter_rows",
    )(me, other, *in_hbm((expert_ids.T, expert_share.T, ffn_input, ffn_gain[None, :])))
    return got[0], got[1:]


def choice(info, expert, per_expert):
    rows = info.shape[0]
    first, second = info[:, 0:1], info[:, 1:2]
    share0 = info[:, 2:3] + info[:, 3:4] + info[:, 4:5]
    share1 = info[:, 5:6] + info[:, 6:7] + info[:, 7:8]
    row_id, col_id = iota((rows, rows), 0), iota((rows, rows), 1)
    has = jnp.where((first == expert) | (second == expert), 1.0, 0.0)
    has_row = to_row(has, row_id == col_id)
    rank_row = jnp.sum(jnp.where(row_id < col_id, has, 0.0), 0, keepdims=True)
    place = iota((per_expert, rows), 0).astype(F32)
    select = jnp.where((rank_row == place) & (has_row > 0.0), 1.0, 0.0).astype(BF16)
    return select, has * jnp.where(first == expert, share0, share1)


def up_kernel(parts, order, per_expert, me_ref, *refs):
    pieces = refs[: parts * len(order)]
    gate_ref, up_ref, hidden_ref, info_ref, slab = refs[parts * len(order) :]
    me = me_ref[0]
    per_part = pieces[0].shape[0]
    width = pieces[0].shape[1] - INFO
    cols = width // per_part
    own_row = iota((per_part, width), 1) // cols == iota((per_part, width), 0)
    place, lane = iota((INFO, width), 0) - GAIN_AT, iota((INFO, width), 1) % cols
    unfold = jnp.where((place >= 0) & (place < 3 * cols) & (place % cols == lane), 1.0, 0.0).astype(BF16)
    squares, gains = None, []
    for n in range(len(order)):
        info = jnp.concatenate([pieces[n * parts + part][:, width:] for part in range(parts)], 0).astype(F32)
        mine = info[:, 8:9] + info[:, 9:10] + info[:, 10:11]
        squares = mine if squares is None else squares + mine
        spread = mm(pieces[n * parts][:, width:], unfold)
        gains.append(jnp.sum(jnp.where(own_row, spread, 0.0), 0, keepdims=True))
        if n == 0:
            own = info
            info_ref[...] = info
    scale = lax.rsqrt(squares * (1.0 / (width * len(order))) + EPSILON)
    for n, r in enumerate(order):
        start = pl.multiple_of((me ^ r) * width, INFO)
        for part in range(parts):
            span = slice(part * per_part, (part + 1) * per_part)
            x = pieces[n * parts + part][:, :width].astype(F32)
            slab[span, pl.ds(start, width)] = (x * scale[span] * gains[n]).astype(BF16)
    for e in range(gate_ref.shape[0]):
        select, _ = choice(own, float(e), per_expert)
        g = mm(slab[...], gate_ref[e])
        u = mm(slab[...], up_ref[e])
        hidden = (g / (1.0 + jnp.exp(-g)) * u).astype(BF16)
        hidden_ref[e * per_expert : (e + 1) * per_expert, :] = mm(select, hidden).astype(BF16)


def expert_up(parts, order, per_expert, me, pieces, w_gate, w_up):
    experts, depth, hidden = w_gate.shape
    rows = pieces[0].shape[0] * parts
    smem, vmem = (pl.BlockSpec(memory_space=s) for s in (pltpu.SMEM, pltpu.VMEM))
    return pl.pallas_call(
        functools.partial(up_kernel, parts, order, per_expert),
        out_shape=(
            jax.ShapeDtypeStruct((experts * per_expert, hidden), BF16),
            jax.ShapeDtypeStruct((rows, INFO), F32),
        ),
        in_specs=[smem] + [vmem] * (len(pieces) + 2),
        scratch_shapes=[pltpu.VMEM((rows, depth), BF16)],
        compiler_params=pltpu.CompilerParams(vmem_limit_bytes=SMALL_VMEM),
        name="expert_up",
    )(me, *pieces, *in_vmem((w_gate, w_up)))


def down_kernel(parts, order, per_expert, me_ref, info_ref, *refs):
    pieces = refs[: len(order)]
    down_ref = refs[len(order)]
    outs = refs[len(order) + 1 : len(order) + 1 + parts]
    slab = refs[-1]
    me = me_ref[0]
    hidden = pieces[0].shape[1]
    for n, r in enumerate(order):
        slab[:, pl.ds(pl.multiple_of((me ^ r) * hidden, 128), hidden)] = pieces[n][...]
    info = info_ref[...]
    total = None
    for e in range(down_ref.shape[0]):
        select, share = choice(info, float(e), per_expert)
        copy = mm(slab[e * per_expert : (e + 1) * per_expert, :], down_ref[e]).astype(BF16)
        term = mm_tn(select, copy) * share
        total = term if total is None else total + term
    per_part = info.shape[0] // parts
    for part in range(parts):
        outs[part][...] = total[part * per_part : (part + 1) * per_part].astype(BF16)


def expert_down(parts, order, per_expert, me, info, pieces, w_down):
    experts, depth, width = w_down.shape
    rows = info.shape[0]
    smem, vmem = (pl.BlockSpec(memory_space=s) for s in (pltpu.SMEM, pltpu.VMEM))
    return pl.pallas_call(
        functools.partial(down_kernel, parts, order, per_expert),
        out_shape=(jax.ShapeDtypeStruct((rows // parts, width), BF16),) * parts,
        in_specs=[smem, vmem] + [vmem] * (len(pieces) + 1),
        scratch_shapes=[pltpu.VMEM((experts * per_expert, depth), BF16)],
        compiler_params=pltpu.CompilerParams(vmem_limit_bytes=SMALL_VMEM),
        name="expert_down",
    )(me, info, *pieces, *in_vmem((w_down,)))


def restore_kernel(perm_ref, *refs):
    *pieces, out_ref = refs
    moved = jnp.concatenate([piece[...] for piece in pieces], 0)
    out_ref[...] = mm_tn(perm_ref[...], moved).astype(BF16)


def restore_rows(perm, pieces):
    return pl.pallas_call(
        restore_kernel,
        out_shape=jax.ShapeDtypeStruct((perm.shape[0], pieces[0].shape[1]), BF16),
        compiler_params=pltpu.CompilerParams(vmem_limit_bytes=SMALL_VMEM),
        name="restore_rows",
    )(perm, *pieces)


def shifted(value, axis, count, step, use_xor, back=False):
    if step == 0:
        return value
    if use_xor:
        pairs = [(i, i ^ step) for i in range(count)]
    else:
        pairs = [(i, (i - step if back else i + step) % count) for i in range(count)]
    return lax.ppermute(value, axis, pairs)


def doubled(pieces, lanes):
    bit = lanes // 2
    while bit:
        moved = []
        for piece in pieces:
            moved.append(shifted(piece, "tp", lanes, bit, True))
        pieces = pieces + moved
        bit //= 2
    return pieces


def along_parts(pieces, parts, back):
    moved = []
    for k, piece in enumerate(pieces):
        moved.append(shifted(piece, "ep", parts, k, is_power(parts), back))
    return moved


def grouped_start(ffn_input, ffn_gain, expert_ids, expert_share, owned):
    parts = lax.axis_size("ep")
    me = lax.axis_index("ep").astype(jnp.int32)[None]
    other = lax.axis_index("tp").astype(jnp.int32)[None]
    perm, sent = scatter_rows(parts, owned, is_power(parts), me, other, expert_ids, expert_share, ffn_input, ffn_gain)
    pieces = along_parts(sent, parts, False)
    return perm, other, doubled(pieces, lax.axis_size("tp"))


def grouped_end(perm, me, pieces, w_gate, w_up, w_down):
    parts, lanes = lax.axis_size("ep"), lax.axis_size("tp")
    per_expert = 2 * perm.shape[0] // w_gate.shape[0]
    order = [0]
    bit = lanes // 2
    while bit:
        order = order + [r ^ bit for r in order]
        bit //= 2
    hidden, info = expert_up(parts, tuple(order), per_expert, me, pieces, w_gate, w_up)
    hiddens = doubled([hidden], lanes)
    back = expert_down(parts, tuple(order), per_expert, me, info, hiddens, w_down)
    return restore_rows(perm, along_parts(back, parts, True))


def spread_experts(ffn_input, ffn_gain, expert_ids, expert_share, w_gate, w_up, w_down):
    floats = ffn_input.astype(F32)
    square_sum = lax.psum(jnp.sum(floats * floats, -1), "tp")
    full_width = ffn_input.shape[1] * lax.axis_size("tp")
    normed = (floats * lax.rsqrt(square_sum / full_width + EPSILON)[:, None] * ffn_gain).astype(BF16)
    pick_count = expert_ids.shape[1]
    flat_ids = expert_ids.reshape(-1)
    sort_order = jnp.argsort(flat_ids, stable=True)
    source_rows = sort_order // pick_count
    experts_local = w_gate.shape[0]
    expert_devices = lax.axis_size("ep")
    capacity = flat_ids.shape[0] // (experts_local * expert_devices)
    outgoing = normed[source_rows].reshape(expert_devices, experts_local, capacity, normed.shape[1])
    arrived = lax.all_to_all(outgoing, "ep", split_axis=0, concat_axis=0, tiled=True)
    slab_in = lax.all_gather(arrived, "tp", axis=3, tiled=True)
    gate_sum = jnp.einsum("secl,elf->secf", slab_in, w_gate, preferred_element_type=F32)
    up_sum = jnp.einsum("secl,elf->secf", slab_in, w_up, preferred_element_type=F32)
    hidden = (jax.nn.silu(gate_sum) * up_sum).astype(BF16)
    merged = jnp.einsum(
        "secf,efd->secd", lax.all_gather(hidden, "tp", axis=3, tiled=True), w_down, preferred_element_type=F32
    )
    copies = merged.astype(BF16)
    returned = lax.all_to_all(copies, "ep", split_axis=0, concat_axis=0, tiled=True).reshape(-1, w_down.shape[2])
    slots = jnp.argsort(sort_order)
    per_slot = returned[slots].reshape(expert_ids.shape[0], pick_count, -1)
    return jnp.sum(per_slot.astype(F32) * expert_share[..., None], axis=1).astype(BF16)


def body(
    mix_query,
    mix_keys,
    mix_values,
    beta_in,
    decay_in,
    norm_gain,
    ffn_input,
    ffn_gain,
    expert_ids,
    expert_share,
    w_gate,
    w_up,
    w_down,
):
    rows, width = ffn_input.shape
    whole_groups = w_gate.shape[0] % GROUP == 0 and is_power(lax.axis_size("tp"))
    packs = width * lax.axis_size("ep") % rows == 0 and GAIN_AT + 3 * width * lax.axis_size("ep") // rows <= INFO
    mixer_args = (mix_query, mix_keys, mix_values, beta_in, decay_in)
    if whole_groups and packs:
        perm, tp_me, pieces = grouped_start(ffn_input, ffn_gain, expert_ids, expert_share, w_gate.shape[0])
        parts, own, near = mixer_start(*mixer_args, (w_gate, w_up), (w_down,))
        ffn_out = grouped_end(perm, tp_me, pieces, *near)
    else:
        parts, own, _ = mixer_start(*mixer_args, (), ())
        ffn_out = spread_experts(ffn_input, ffn_gain, expert_ids, expert_share, w_gate, w_up, w_down)
    mix_out = mixer_end(parts, own, norm_gain)
    return (mix_out, ffn_out)


def solution(mesh):
    placed = (
        P(("grp", "ep"), "tp", None),
        P(("grp", "ep"), "tp", None),
        P(("grp", "ep"), "tp", None),
        P("tp", ("grp", "ep")),
        P("tp", ("grp", "ep")),
        P(),
        P(("grp", "ep"), "tp"),
        P("tp"),
        P(("grp", "ep"), None),
        P(("grp", "ep"), None),
        P("ep", None, "tp"),
        P("ep", None, "tp"),
        P("ep", None, "tp"),
    )
    return jax.shard_map(
        body,
        mesh=mesh,
        in_specs=placed,
        out_specs=(P(("grp", "ep"), "tp", None), P(("grp", "ep"), "tp")),
        check_vma=False,
    )
```
